32 devices in a mesh: row: 8 (over z, x), col: 4 (over y, core).
Axes of the slice: x: 2, y: 2, z: 4, core: 2. Of those that a mesh axis runs over, the one named last changes fastest.
Arguments:
- tokens: bfloat16 [2, 32768, 2048], P(None, ('row', 'col')), may hold values from -6 to 6
- norm_gain: float32 [2048], replicated, may hold values from 0.1 to 1.9
- mix_weight: bfloat16 [2048, 1024], replicated, may hold values from -0.125 to 0.125
- gate_weight: bfloat16 [2048, 2048], replicated, may hold values from -0.125 to 0.125
- out_weight: bfloat16 [1024, 2048], replicated, may hold values from -0.1875 to 0.1875
Outputs:
- gated: bfloat16 [2, 32768, 2048], P(None, ('row', 'col'))
The draws below stay inside these ranges and needn't reach their ends.
All inputs are finite; a program needn't handle non-finite values.
Results may differ from the reference program's by a relative error of at most 0.017.
Values may be sent and summed in bfloat16 or wider, within the bound.
A program may use at most 128 MiB of HBM per device.

```python
import jax
import jax.numpy as jnp
from jax import lax

D = 2048
GROUPS = 8
GROUP_DIM = 128
FW = 1024
LENGTH = 32768
SEQS = 2


def steps_of(key, dims, split, low, high):
    gain, own = 1.0, jax.random.fold_in(key, 6)
    for dim, shards_of in split:
        steps = jnp.exp(jax.random.uniform(jax.random.fold_in(own, dim), (shards_of,), jnp.float32, low / len(split), high / len(split)))
        gain = gain * jnp.repeat(steps, dims[dim] // shards_of).reshape([-1 if axis == dim else 1 for axis in range(len(dims))])
    return gain


def bell_draw(key, dims, spread, reach, split=(), dtype=jnp.bfloat16):
    loudness = steps_of(key, dims, split, -0.22, 0.18) if split else 1.0
    entries = jax.random.normal(key, dims, jnp.float32) * spread * loudness
    return jnp.minimum(jnp.maximum(entries, -reach), reach).astype(dtype)


def setup_inputs(seed: int = 0) -> dict:
    streams_of = jax.random.split(jax.random.key(seed), 6)
    tokens = bell_draw(streams_of[0], (SEQS, LENGTH, D), 1.0, 6.0, ((1, 32),))
    norm_gain = jnp.clip(1.0 + 0.18 * jax.random.normal(streams_of[1], (D,), jnp.float32), 0.1, 1.9)
    mix_weight = bell_draw(streams_of[2], (D, FW), D ** -0.5, 0.125)
    gate_weight = bell_draw(streams_of[3], (D, D), D ** -0.5, 0.125)
    out_weight = bell_draw(streams_of[4], (FW, D), FW ** -0.5, 0.1875)
    return {"tokens": tokens, "norm_gain": norm_gain, "mix_weight": mix_weight, "gate_weight": gate_weight, "out_weight": out_weight}


def reference(tokens, norm_gain, mix_weight, gate_weight, out_weight):

    def one_sequence(sequence):
        widened = sequence.astype(jnp.float32)
        inverse_rms = lax.rsqrt(lax.optimization_barrier(jnp.mean(widened * widened, axis=-1, keepdims=True)) + 1e-06)
        normed = (widened * inverse_rms * norm_gain.astype(jnp.float32)).astype(jnp.bfloat16)
        mixed_in = jnp.dot(normed, mix_weight, preferred_element_type=jnp.float32).astype(jnp.bfloat16)
        gate_value = jax.nn.sigmoid(jnp.dot(normed, gate_weight, preferred_element_type=jnp.float32))
        grouped = mixed_in.astype(jnp.float32).reshape(LENGTH, GROUPS, GROUP_DIM)
        spectrum = jnp.fft.fft2(grouped, axes=(0, 2), norm='ortho').real
        spectral = spectrum.reshape(LENGTH, GROUPS * GROUP_DIM).astype(jnp.bfloat16)
        mapped = jnp.dot(spectral, out_weight, preferred_element_type=jnp.float32)
        return (gate_value * mapped).astype(jnp.bfloat16)
    return lax.map(one_sequence, tokens)
```

```python
import functools
import math

import jax
import jax.numpy as jnp
import numpy as np
from jax import lax
from jax.experimental import pallas as pl
from jax.experimental.pallas import tpu as pltpu
from jax.sharding import PartitionSpec as P

GROUP_DIM = 128
HALF = GROUP_DIM // 2
BF16 = jnp.bfloat16
F32 = jnp.float32
AXES = ("row", "col")


def angles(left, right, period):
    return (np.outer(left, right) % period) * (2.0 * math.pi / period)


def channel_table():
    phase = angles(np.arange(GROUP_DIM), np.arange(HALF), GROUP_DIM)
    table = np.stack([np.cos(phase), np.sin(phase)], axis=-1)
    table[:, 0, 1] = np.cos(math.pi * np.arange(GROUP_DIM))
    return table.reshape(GROUP_DIM, GROUP_DIM) * GROUP_DIM ** -0.5


def channel_order():
    order = np.zeros((HALF, 2), np.int64)
    order[:, 0] = np.arange(HALF)
    order[:, 1] = GROUP_DIM - np.arange(HALF)
    order[0, 1] = HALF
    pick = np.zeros((GROUP_DIM, GROUP_DIM))
    pick[np.arange(GROUP_DIM), order.reshape(-1)] = 1.0
    return pick


def position_tables(devices, length, first):
    second, fold = length // first, first // devices
    phase = angles(np.arange(first), np.arange(first), first)
    cosine, sine = np.cos(phase), np.sin(phase)
    zero = np.zeros_like(cosine)
    from_left = np.concatenate([cosine, sine, cosine, sine], axis=1)
    from_right = np.concatenate([-sine, cosine, sine, -cosine], axis=1)
    lone_left = np.concatenate([cosine, sine, zero, zero], axis=1)
    lone_right = np.concatenate([zero, zero, cosine, sine], axis=1)

    def interleave(left, right):
        pair = np.stack([left.reshape(devices, fold, -1), right.reshape(devices, fold, -1)], axis=1)
        return pair.reshape(2 * first, 4 * first)

    turn = angles(np.arange(second), np.arange(first), length)
    last = angles(np.arange(second), np.arange(second), second)
    closing = np.concatenate([np.cos(last), -np.sin(last)], axis=1) * length ** -0.5
    return (
        interleave(from_left, from_right),
        interleave(lone_left, lone_right),
        np.cos(turn),
        np.sin(turn),
        closing,
    )


def transform_kernel(first, direct, x_ref, g_ref, cos_ref, sin_ref, close_ref, out_ref):
    cosine, sine = cos_ref[...], sin_ref[...]
    seqs = x_ref.shape[2] if direct else x_ref.shape[1]
    for seq in range(seqs):
        if direct:
            x = x_ref[:, 0, seq].reshape(2 * first, x_ref.shape[-1])
        else:
            x = x_ref[0, seq]
        u = lax.dot_general(x, g_ref[0], (((0,), (0,)), ((), ())), preferred_element_type=F32)
        halves = []
        for half in range(2):
            real = u[:, 2 * half * first : (2 * half + 1) * first]
            imag = u[:, (2 * half + 1) * first : (2 * half + 2) * first]
            turned = jnp.concatenate(
                [(real * cosine - imag * sine).astype(BF16), (real * sine + imag * cosine).astype(BF16)], axis=0
            )
            halves.append(turned)
        turned = jnp.concatenate(halves, axis=1)
        y = jnp.dot(close_ref[...], turned, preferred_element_type=F32)
        if direct:
            out_ref[:, seq] = y.reshape(out_ref.shape[0], out_ref.shape[2], out_ref.shape[3]).astype(BF16)
        else:
            out_ref[seq] = y.astype(BF16)


def position_transform(x, lone_here, devices, length, first):
    _, pairs, seqs, rows, second = x.shape
    normal, lone, cosine, sine, closing = position_tables(devices, length, first)
    normal, lone = jnp.asarray(normal, BF16), jnp.asarray(lone, BF16)
    g = jnp.stack([jnp.where(lone_here, lone, normal), normal])
    direct = rows % 8 == 0 and second // devices >= 8
    if direct:
        x_spec = pl.BlockSpec((devices, 1, seqs, rows, second), lambda p: (0, p, 0, 0, 0))
        out_shape = (devices, seqs, second // devices, pairs * 2 * first)
        out_spec = pl.BlockSpec((devices, seqs, second // devices, 2 * first), lambda p: (0, 0, 0, p))
    else:
        x = x.transpose(1, 2, 0, 3, 4).reshape(pairs, seqs, devices * rows, second)
        x_spec = pl.BlockSpec((1, seqs, devices * rows, second), lambda p: (p, 0, 0, 0))
        out_shape = (seqs, second, pairs * 2 * first)
        out_spec = pl.BlockSpec((seqs, second, 2 * first), lambda p: (0, 0, p))
    whole = lambda p: (0, 0)
    y = pl.pallas_call(
        functools.partial(transform_kernel, first, direct),
        grid=(pairs,),
        in_specs=[
            x_spec,
            pl.BlockSpec((1, 2 * first, 4 * first), lambda p: (jnp.minimum(p, 1), 0, 0)),
            pl.BlockSpec((second, first), whole),
            pl.BlockSpec((second, first), whole),
            pl.BlockSpec((second, 2 * second), whole),
        ],
        out_specs=out_spec,
        out_shape=jax.ShapeDtypeStruct(out_shape, BF16),
        compiler_params=pltpu.CompilerParams(dimension_semantics=("arbitrary",)),
        cost_estimate=pl.CostEstimate(
            flops=pairs * seqs * second * first * 16 * (first + second), bytes_accessed=4 * x.size, transcendentals=0
        ),
    )(x, g, jnp.asarray(cosine, F32), jnp.asarray(sine, F32), jnp.asarray(closing, BF16))
    if direct:
        return y
    here = length // devices
    width = min(first, here)
    y = y.reshape(seqs, devices, here // width, -1, pairs * 2, width) if first <= here else (
        y.reshape(seqs, second, pairs * 2, first // here, here).transpose(0, 1, 3, 2, 4)
        .reshape(seqs, devices, 1, 1, pairs * 2, here)
    )
    return y.reshape(seqs, devices, here // width, -1).transpose(1, 0, 2, 3)


def local(devices, tokens, norm_gain, mix_weight, gate_weight, out_weight):
    seqs, here, width = tokens.shape
    length = here * devices
    mixed = mix_weight.shape[1]
    groups = mixed // GROUP_DIM
    pairs = mixed // devices // 2
    first = max(GROUP_DIM, devices)
    fold = first // devices
    second = length // first

    mix = jnp.einsum(
        "dgj,jk->dgk", mix_weight.reshape(width, groups, GROUP_DIM), jnp.asarray(channel_table(), BF16),
        preferred_element_type=F32,
    ).astype(BF16).reshape(width, mixed)
    widened = tokens.astype(F32)
    inverse_rms = lax.rsqrt(jnp.mean(widened * widened, axis=-1, keepdims=True) + 1e-06)
    normed = (widened * inverse_rms * norm_gain).astype(BF16)
    columns = lax.dot_general(
        mix, normed, (((0,), (2,)), ((), ())), preferred_element_type=F32
    ).astype(BF16)
    sent = columns.reshape(devices, pairs, 2, seqs, fold, second).transpose(0, 1, 3, 2, 4, 5)
    sent = sent.reshape(devices, pairs, seqs, 2 * fold, second)
    arrived = lax.all_to_all(sent, AXES, split_axis=0, concat_axis=0, tiled=True)

    gate_value = jax.nn.sigmoid(jnp.dot(normed, gate_weight, preferred_element_type=F32)).astype(BF16)
    ordered = jnp.einsum(
        "ij,gjd->gid", jnp.asarray(channel_order(), BF16), out_weight.reshape(groups, GROUP_DIM, width),
        preferred_element_type=F32,
    ).astype(BF16).reshape(mixed, width)
    gate_value, ordered, arrived = lax.optimization_barrier((gate_value, ordered, arrived))

    lone_here = lax.axis_index(AXES) * pairs % HALF == 0
    spectra = position_transform(arrived, lone_here, devices, length, first)
    returned = lax.all_to_all(spectra, AXES, split_axis=0, concat_axis=0, tiled=True)
    span = min(first, here)
    returned = returned.reshape(devices, seqs, here // span, 2 * pairs, span)
    spectral = returned.transpose(1, 2, 4, 0, 3).reshape(seqs, here, mixed)
    mapped = jnp.dot(spectral, ordered, preferred_element_type=F32)
    return (gate_value * mapped).astype(BF16)


def solution(mesh):
    in_specs = (P(None, AXES, None), P(), P(), P(), P())
    devices = mesh.shape["row"] * mesh.shape["col"]
    body = functools.partial(local, devices)
    return jax.shard_map(body, mesh=mesh, in_specs=in_specs, out_specs=P(None, AXES, None), check_vma=False)
```

```python
import functools
import math

import jax
import jax.numpy as jnp
import numpy as np
from jax import lax
from jax.experimental import pallas as pl
from jax.experimental.pallas import tpu as pltpu
from jax.sharding import PartitionSpec as P

GROUP_DIM = 128
HALF = GROUP_DIM // 2
BF16 = jnp.bfloat16
F32 = jnp.float32
AXES = ("row", "col")
LANES = 128
STEP = 8


def angles(left, right, period):
    return (np.outer(left, right) % period) * (2.0 * math.pi / period)


def channel_table():
    phase = angles(np.arange(GROUP_DIM), np.arange(HALF), GROUP_DIM)
    table = np.stack([np.cos(phase), np.sin(phase)], axis=-1)
    table[:, 0, 1] = np.cos(math.pi * np.arange(GROUP_DIM))
    return table.reshape(GROUP_DIM, GROUP_DIM) * GROUP_DIM ** -0.5


def channel_order():
    order = np.zeros((HALF, 2), np.int64)
    order[:, 0] = np.arange(HALF)
    order[:, 1] = GROUP_DIM - np.arange(HALF)
    order[0, 1] = HALF
    pick = np.zeros((GROUP_DIM, GROUP_DIM))
    pick[np.arange(GROUP_DIM), order.reshape(-1)] = 1.0
    return pick


def position_tables(devices, length, first):
    second, fold = length // first, first // devices
    phase = angles(np.arange(first), np.arange(first), first)
    cosine, sine = np.cos(phase), np.sin(phase)
    zero = np.zeros_like(cosine)
    from_left = np.concatenate([cosine, sine, cosine, sine], axis=1)
    from_right = np.concatenate([-sine, cosine, sine, -cosine], axis=1)
    lone_left = np.concatenate([cosine, sine, zero, zero], axis=1)
    lone_right = np.concatenate([zero, zero, cosine, sine], axis=1)

    def interleave(left, right):
        pair = np.stack([left, right]).reshape(2, devices, fold, -1).transpose(0, 2, 1, 3)
        return pair.reshape(2 * first, 4 * first)

    turn = angles(np.arange(second), np.arange(first), length)
    last = angles(np.arange(second), np.arange(second), second)
    closing = np.concatenate([np.cos(last), -np.sin(last)], axis=1) * length ** -0.5
    return (
        interleave(from_left, from_right),
        interleave(lone_left, lone_right),
        np.cos(turn),
        np.sin(turn),
        closing,
    )


def turn_halves(u, cosine, sine, first):
    halves = []
    for half in range(2):
        real = u[..., 2 * half * first : (2 * half + 1) * first]
        imag = u[..., (2 * half + 1) * first : (2 * half + 2) * first]
        halves.append(
            jnp.concatenate(
                [(real * cosine - imag * sine).astype(BF16), (real * sine + imag * cosine).astype(BF16)], axis=-2
            )
        )
    return jnp.concatenate(halves, axis=-1)


def transform_kernel(first, x_ref, g_ref, cos_ref, sin_ref, close_ref, out_ref, rows_in, rows_out):
    devices, channels, here = x_ref.shape
    second = cos_ref.shape[0]
    fold, tiles = here // second, second // LANES
    for tile in range(here // LANES):
        rows_in[tile] = (
            x_ref[:, :, tile * LANES : (tile + 1) * LANES].astype(F32).reshape(devices * channels, LANES)
        )
    cosine, sine = cos_ref[...], sin_ref[...]
    for pair in range(channels // 2):
        rows = []
        for column in range(2):
            for high in range(fold):
                picked = pl.ds(2 * pair + column, devices, stride=channels)
                rows.append(
                    jnp.concatenate(
                        [rows_in[high * tiles + tile, picked, :] for tile in range(tiles)], axis=1
                    ).astype(BF16)
                )
        x = jnp.concatenate(rows, axis=0)
        g = g_ref[0] if pair == 0 else g_ref[1]
        if pair == 0:
            g = jnp.where(pl.program_id(0) == 0, g, g_ref[1])
        u = lax.dot_general(x, g, (((0,), (0,)), ((), ())), preferred_element_type=F32)
        turned = turn_halves(u, cosine, sine, first)
        y = jnp.dot(close_ref[...], turned, preferred_element_type=F32)
        for half in range(2):
            rows_out[pl.ds(2 * pair + half, second, stride=channels), :] = y[:, half * first : (half + 1) * first]
    out_ref[...] = rows_out[...].reshape(out_ref.shape).astype(BF16)


def position_transform(x, lone_here, devices, length, first):
    _, channels, here = x.shape
    second, fold = length // first, first // devices
    normal, lone, cosine, sine, closing = position_tables(devices, length, first)
    normal, lone = jnp.asarray(normal, BF16), jnp.asarray(lone, BF16)
    cosine, sine, closing = jnp.asarray(cosine, F32), jnp.asarray(sine, F32), jnp.asarray(closing, BF16)
    g = jnp.stack([jnp.where(lone_here, lone, normal), normal])
    if not fits(channels, here, first, devices):
        pairs, span = channels // 2, min(first, here)
        x = x.reshape(devices, pairs, 2, fold, second).transpose(1, 2, 3, 0, 4).reshape(pairs, 2 * first, second)
        g = jnp.stack([g[min(pair, 1)] for pair in range(pairs)])
        u = jnp.einsum("pxr,pxj->prj", x, g, preferred_element_type=F32)
        y = jnp.einsum("kx,pxj->pkj", closing, turn_halves(u, cosine, sine, first), preferred_element_type=F32)
        y = y.astype(BF16).reshape(pairs, second, 2, first).transpose(1, 3, 0, 2)
        return y.reshape(devices, here // span, span, channels).transpose(0, 1, 3, 2)
    low = second // devices
    whole = lambda step: (0, 0)
    return pl.pallas_call(
        functools.partial(transform_kernel, first),
        grid=(channels // STEP,),
        in_specs=[
            pl.BlockSpec((devices, STEP, here), lambda step: (0, step, 0)),
            pl.BlockSpec((2, 2 * first, 4 * first), lambda step: (0, 0, 0)),
            pl.BlockSpec((second, first), whole),
            pl.BlockSpec((second, first), whole),
            pl.BlockSpec((second, 2 * second), whole),
        ],
        out_specs=pl.BlockSpec((devices, low, STEP, first), lambda step: (0, 0, step, 0)),
        out_shape=jax.ShapeDtypeStruct((devices, low, channels, first), BF16),
        scratch_shapes=[
            pltpu.VMEM((here // LANES, devices * STEP, LANES), F32),
            pltpu.VMEM((second * STEP, first), F32),
        ],
        compiler_params=pltpu.CompilerParams(dimension_semantics=("arbitrary",)),
        cost_estimate=pl.CostEstimate(
            flops=channels * second * first * 8 * (first + second), bytes_accessed=4 * x.size, transcendentals=0
        ),
    )(x, g, cosine, sine, closing)


def fits(channels, here, first, devices):
    return first == LANES and channels % STEP == 0 and devices % 16 == 0 and here % (2 * first) == 0


def closing_kernel(r_ref, w_ref, gate_ref, *rest):
    out_ref = rest[-1]
    mixed = w_ref.shape[0]
    span = r_ref.shape[3]
    left = jnp.concatenate([r_ref[:, low].reshape(mixed, span) for low in range(r_ref.shape[1])], axis=1)
    mapped = lax.dot_general(left, w_ref[...], (((0,), (0,)), ((), ())), preferred_element_type=F32)
    out_ref[0] = (gate_ref[0].astype(F32) * mapped).astype(BF16)


def close(seq, returned, ordered, gate_value, so_far):
    devices, lows, channels, span = returned.shape
    seqs, here, width = gate_value.shape
    mixed = ordered.shape[0]
    many = 2
    block = pl.BlockSpec((1, many * span, width), lambda step: (seq, step, 0))
    operands = [returned, ordered, gate_value]
    in_specs = [
        pl.BlockSpec((devices, many, channels, span), lambda step: (0, step, 0, 0)),
        pl.BlockSpec((mixed, width), lambda step: (0, 0)),
        block,
    ]
    if so_far is not None:
        operands.append(so_far)
        in_specs.append(pl.BlockSpec(memory_space=pl.ANY))
    return pl.pallas_call(
        closing_kernel,
        grid=(lows // many,),
        in_specs=in_specs,
        out_specs=block,
        out_shape=jax.ShapeDtypeStruct((seqs, here, width), BF16),
        input_output_aliases={} if so_far is None else {3: 0},
        compiler_params=pltpu.CompilerParams(dimension_semantics=("arbitrary",)),
        cost_estimate=pl.CostEstimate(
            flops=2 * here * mixed * width, bytes_accessed=2 * (here * mixed + mixed * width + 2 * here * width),
            transcendentals=0,
        ),
    )(*operands)


def local(devices, tokens, norm_gain, mix_weight, gate_weight, out_weight):
    seqs, here, width = tokens.shape
    length = here * devices
    mixed = mix_weight.shape[1]
    groups = mixed // GROUP_DIM
    channels = mixed // devices
    first = max(GROUP_DIM, devices)
    span = min(first, here)

    mix = jnp.einsum(
        "dgj,jk->dgk", mix_weight.reshape(width, groups, GROUP_DIM), jnp.asarray(channel_table(), BF16),
        preferred_element_type=F32,
    ).astype(BF16).reshape(width, mixed)

    def norm(x):
        widened = x.astype(F32)
        inverse_rms = lax.rsqrt(jnp.mean(widened * widened, axis=-1, keepdims=True) + 1e-06)
        return (widened * inverse_rms * norm_gain).astype(BF16)

    def exchange(x):
        return lax.all_to_all(x, AXES, split_axis=0, concat_axis=0, tiled=True)

    lone_here = lax.axis_index(AXES) * (channels // 2) % HALF == 0
    transform = functools.partial(
        position_transform, lone_here=lone_here, devices=devices, length=length, first=first
    )
    arrived = []
    for seq in range(seqs):
        columns = lax.dot_general(
            mix, norm(tokens[seq]), (((0,), (1,)), ((), ())), preferred_element_type=F32
        ).astype(BF16).reshape(devices, channels, here)
        if seq:
            columns, arrived[-1] = lax.optimization_barrier((columns, arrived[-1]))
        arrived.append(exchange(columns))

    gate_value = jax.nn.sigmoid(jnp.dot(norm(tokens), gate_weight, preferred_element_type=F32)).astype(BF16)
    ordered = jnp.einsum(
        "ij,gjd->gid", jnp.asarray(channel_order(), BF16), out_weight.reshape(groups, GROUP_DIM, width),
        preferred_element_type=F32,
    ).astype(BF16).reshape(mixed, width)
    gate_value, ordered, arrived[-1] = lax.optimization_barrier((gate_value, ordered, arrived[-1]))

    returned = []
    for seq in range(seqs):
        spectra = transform(arrived[seq])
        if seq:
            spectra, returned[-1] = lax.optimization_barrier((spectra, returned[-1]))
        returned.append(exchange(spectra))

    if fits(channels, here, first, devices):
        gated = None
        for seq in range(seqs):
            gated = close(seq, returned[seq], ordered, gate_value, gated)
        return gated
    spectral = jnp.stack(returned).transpose(0, 2, 4, 1, 3).reshape(seqs, here, mixed)
    mapped = jnp.dot(spectral, ordered, preferred_element_type=F32)
    return (gate_value * mapped).astype(BF16)


def solution(mesh):
    in_specs = (P(None, AXES, None), P(), P(), P(), P())
    devices = mesh.shape["row"] * mesh.shape["col"]
    body = functools.partial(local, devices)
    return jax.shard_map(body, mesh=mesh, in_specs=in_specs, out_specs=P(None, AXES, None), check_vma=False)
```
